256 devices in a mesh: grp: 2 (over y), fs: 16 (over z), tp: 8 (over x, core).
Axes of the slice: x: 4, y: 2, z: 16, core: 2. Of those that a mesh axis runs over, the one named last changes fastest.
The devices are a block of a 4x16x16 slice.
Arguments:
- tokens: bfloat16 [32768, 2048], P(('grp', 'fs', 'tp')), parts along dimension 0, may hold values from -12 to 12
- norm_gain: float32 [2048], replicated, may hold values from 0.1 to 1.9
- w_in: bfloat16 [2048, 8192], P('fs', 'tp'), may hold values from -0.125 to 0.125
- w_out: bfloat16 [8192, 2048], P('tp', 'fs'), may hold values from -0.0625 to 0.0625
Outputs:
- mixed: bfloat16 [32768, 2048], P(('grp', 'fs', 'tp')), parts along dimension 0
The draws below stay inside these ranges and needn't reach their ends.
There are 2 independent parts, one for each index of `grp`. The reference program is written for one: setup_inputs(seed, part) draws one part's arguments, and reference() takes and returns one part's arrays. A program takes and returns all parts, laid end to end along the dimension named above; an argument that names none is the same for every part. Nothing has to cross between parts.
All inputs are finite; a program needn't handle non-finite values.
Results may differ from the reference program's by a relative error of at most 0.012.
Values may be sent and summed in bfloat16 or wider, within the bound.
A program may use at most 64 MiB of HBM per device.

```python
import math
import jax
import jax.numpy as jnp
from jax import lax

D = 2048
FF = 8192
FF_DEV = 1024
TOKENS = 16384
N_TP = 8


def draw_tokens(key, part):
    first = jax.random.fold_in(key, 11)
    second = jax.random.fold_in(key, 12)
    scales = jnp.exp(jax.random.uniform(second, (TOKENS, 1), jnp.float32, math.log(0.35), math.log(2.8)))
    base = jax.random.normal(first, (TOKENS, D), jnp.float32)
    return jnp.clip(base * scales, -12.0, 12.0).astype(jnp.bfloat16)


def block_scale(stream_key, extent, cuts, low, top_value):
    gain, own = 1.0, jax.random.fold_in(stream_key, 6)
    for position, shards_of in cuts:
        steps = jnp.exp(jax.random.uniform(jax.random.fold_in(own, position), (shards_of,), jnp.float32, low / len(cuts), top_value / len(cuts)))
        gain = gain * jnp.repeat(steps, extent[position] // shards_of).reshape([-1 if axis == position else 1 for axis in range(len(extent))])
    return gain


def gaussian(rng, dims, spread, bound, cuts=(), dtype=jnp.bfloat16):
    entries = jax.random.normal(rng, dims, jnp.float32) * spread
    if len(cuts) > 0:
        entries = block_scale(rng, dims, cuts, -0.22, 0.18) * entries
    return jnp.clip(entries, min=-bound, max=bound).astype(dtype)


def setup_inputs(seed: int = 0, part: int = 0) -> dict:
    key_list = jax.random.split(jax.random.key(seed), 5)
    own_keys = jax.random.split(jax.random.fold_in(key_list[4], part), 5)
    tokens = draw_tokens(jax.random.fold_in(jax.random.fold_in(key_list[4], part), 71), part)
    norm_gain = jnp.clip(1.0 + 0.18 * jax.random.normal(key_list[1], (D,), jnp.float32), 0.1, 1.9)
    w_in = gaussian(key_list[2], (D, FF), D ** -0.5, 0.125, ((0, 16), (1, 8)))
    w_out = gaussian(key_list[3], (FF, D), FF ** -0.5, 0.0625, ((0, 8), (1, 16)))
    return dict(tokens=tokens, norm_gain=norm_gain, w_in=w_in, w_out=w_out)


EPS = 1e-06

def reference(tokens, norm_gain, w_in, w_out):
    block = math.gcd(TOKENS, 2048)
    pieces = tokens.reshape(TOKENS // block, block, D)

    def one_block(rows_in):
        xf = rows_in.astype(jnp.float32)
        scale = lax.rsqrt(lax.optimization_barrier(jnp.mean(xf * xf, axis=-1, keepdims=True)) + EPS)
        normed = (xf * scale * norm_gain.astype(jnp.float32)).astype(jnp.bfloat16)
        pre = jnp.dot(normed, w_in, preferred_element_type=jnp.float32)
        hidden = jnp.square(jax.nn.relu(pre)).astype(jnp.bfloat16)
        total = xf
        for index in range(N_TP):
            lower = index * FF_DEV
            partial_sum = jnp.dot(hidden[:, lower:lower + FF_DEV], w_out[lower:lower + FF_DEV, :], preferred_element_type=jnp.float32).astype(jnp.bfloat16)
            partial_sum = lax.optimization_barrier(partial_sum)
            total = total + partial_sum.astype(jnp.float32)
        return total.astype(jnp.bfloat16)
    mixed = lax.map(one_block, pieces)
    return mixed.reshape(TOKENS, D)
```

```python
import functools

import jax
import jax.numpy as jnp
from jax import lax
from jax.experimental import pallas as pl
from jax.experimental.pallas import tpu as pltpu
from jax.sharding import PartitionSpec as P

EPS = 1e-06
F32, BF16 = jnp.float32, jnp.bfloat16
MESH = pl.DeviceIdType.MESH
IN_SHARED, OUT_SHARED = 3, 19


def kernel(n, tok_ref, gain_ref, win_ref, wout_ref, out_ref,
           normed, win_all, wout_all, acc, hidden,
           s1_send, s1_keep, d_recv, r1_send, l1_send, l1_recv, r1_recv, r2_send, l2_send, l2_recv, r2_recv,
           zs, zr, ys, yr, ts, tr, ds_, dr, s1s, s1r, xs, xr):
    half = n // 2
    g, z, t = lax.axis_index("grp"), lax.axis_index("fs"), lax.axis_index("tp")
    par = lax.rem(g, 2)
    partner = g + 1 - 2 * par
    x, c = t // 2, lax.rem(t, 2)
    oc = 1 - c
    xr_, xl_, xf_ = lax.rem(x + 1, 4), lax.rem(x + 3, 4), lax.rem(x + 2, 4)
    z_right, z_left = {"fs": lax.rem(z + 1, n)}, {"fs": lax.rem(z + n - 1, n)}
    x_right, x_left, sib = {"tp": 2 * xr_ + c}, {"tp": 2 * xl_ + c}, {"tp": 2 * x + oc}
    peer = {"grp": partner}
    tb, d = tok_ref.shape
    hb = tb // 2
    kb, ff = win_ref.shape
    cb = wout_ref.shape[1]
    started = []

    def remote(src, dst, send, recv, dev):
        return pltpu.make_async_remote_copy(
            src_ref=src, dst_ref=dst, send_sem=send, recv_sem=recv, device_id=dev, device_id_type=MESH)

    def go(copy):
        copy.start()
        started.append(copy)

    barrier = pltpu.get_barrier_semaphore()
    for dev in (z_right, z_left, x_right, x_left, sib, peer):
        pl.semaphore_signal(barrier, inc=1, device_id=dev, device_id_type=MESH)
    pl.semaphore_wait(barrier, 6)

    hops = ((half, half - 1), (half - 1, half))
    own, alls = (win_ref, wout_ref), (win_all, wout_all)
    b_in, b_out = IN_SHARED * 128, OUT_SHARED * 16
    a_in, a_out = ff - 2 * b_in, ff - 2 * b_out

    def slot(direction, k):
        return lax.rem(z - k + n, n) if direction == 0 else lax.rem(z + k, n)

    def region(w, piece, who):
        a, b, unit = ((a_in, b_in, 128), (a_out, b_out, 16))[w]
        part = pl.ds(0, a) if piece == 0 else pl.ds(pl.multiple_of(a + who * b, unit), b)
        return (slice(None), part) if w == 0 else (part, slice(None))

    def hop(w, direction, k, piece):
        s = slot(direction, k - 1)
        r = region(w, piece, par)
        dst = alls[w].at[(s, *r)]
        src = own[w].at[r] if k == 1 else dst
        return remote(src, dst, zs.at[w, direction, k - 1, piece], zr.at[w, direction, k - 1, piece],
                      (z_right, z_left)[direction])

    def hop_recv(w, direction, k, piece):
        ref = alls[w].at[(slot(direction, k), *region(w, piece, par))]
        remote(ref, ref, zs.at[w, direction, k - 1, piece], zr.at[w, direction, k - 1, piece],
               (z_right, z_left)[direction]).wait_recv()

    def share(w, direction, k, who):
        ref = alls[w].at[(slot(direction, k), *region(w, 1, who))]
        return remote(ref, ref, ys.at[w, direction, k - 1], yr.at[w, direction, k - 1], peer)

    def ring_own(w):
        for piece in (1, 0):
            for direction in (0, 1):
                go(hop(w, direction, 1, piece))

    def ring_slot(w, k):
        for piece in (1, 0):
            for direction in (0, 1):
                if k > hops[w][direction]:
                    continue
                hop_recv(w, direction, k, piece)
                if k < hops[w][direction]:
                    go(hop(w, direction, k + 1, piece))
                if piece == 1:
                    go(share(w, direction, k, par))

    def share_wait(w, k):
        for direction in (0, 1):
            if k <= hops[w][direction]:
                share(w, direction, k, 1 - par).wait_recv()

    ring_own(0)

    xf = tok_ref[...].astype(F32)
    scale = lax.rsqrt(jnp.mean(xf * xf, axis=-1, keepdims=True) + EPS)
    normed[c, x] = (xf * scale * gain_ref[...]).astype(BF16)
    acc[...] = jnp.zeros_like(acc)

    def rows(core, chip, h):
        return normed.at[core, chip, pl.ds(h * hb, hb)]

    def tok_send(direction, step):
        chip = x if step < 2 else (xl_, xr_)[direction]
        h = (0, 1, 0)[step] if direction == 0 else (1, 0, 1)[step]
        ref = rows(c, chip, h)
        return remote(ref, ref, ts.at[direction, step], tr.at[direction, step], (x_right, x_left)[direction])

    def tok_ref_in(core, direction, step):
        chip = ((xl_, xr_)[direction], (xl_, xr_)[direction], xf_)[step]
        h = (0, 1, 0)[step] if direction == 0 else (1, 0, 1)[step]
        return rows(core, chip, h)

    def tok_recv(direction, step):
        ref = tok_ref_in(c, direction, step)
        remote(ref, ref, ts.at[direction, step], tr.at[direction, step], (x_right, x_left)[direction]).wait_recv()

    def sib_copy(core, direction, step):
        ref = tok_ref_in(core, direction, step)
        return remote(ref, ref, ds_.at[direction, step], dr.at[direction, step], sib)

    def sib_own(core):
        ref = normed.at[core, x]
        return remote(ref, ref, ds_.at[0, 3], dr.at[0, 3], sib)

    for step in (0, 1):
        for direction in (0, 1):
            go(tok_send(direction, step))
    go(sib_own(c))

    def tok_slot(step):
        for direction in (0, 1):
            tok_recv(direction, step)
            if step == 0:
                go(tok_send(direction, 2))
            go(sib_copy(c, direction, step))

    def tok_wait(step):
        for direction in (0, 1):
            sib_copy(oc, direction, step).wait_recv()

    def product(chip, sa, sb, ra, rb):
        ca = pl.ds(pl.multiple_of(sa * kb, kb), kb)
        cb_ = pl.ds(pl.multiple_of(sb * kb, kb), kb)
        lhs = jnp.concatenate([normed[:, chip, :, ca], normed[:, chip, :, cb_]], axis=-1)
        rhs = jnp.concatenate([ra, rb], axis=0)
        return jnp.dot(lhs.reshape(2 * tb, 2 * kb), rhs, preferred_element_type=F32).reshape(2, tb, ff)

    def pre_add(chips, lo, hi):
        def step(j, _):
            sa, sb = lax.rem(z - j + n, n), lax.rem(z + j, n)
            for chip in chips:
                acc[:, chip] += product(chip, sa, sb, win_all[sa], win_all[sb])
            return 0
        if hi > lo:
            lax.fori_loop(lo, hi, step, 0)

    def finish_hidden():
        far = lax.rem(z + half, n)

        def step(chip, _):
            pre = acc[:, chip] + product(chip, z, far, win_ref[...], win_all[far])
            hidden[:, chip] = jnp.square(jnp.maximum(pre, 0.0)).astype(BF16)
            return 0
        lax.fori_loop(0, 4, step, 0)

    def width(q):
        return cb if q in (0, half) else 2 * cb

    def w_slice(q):
        return pl.ds(0, width(q))

    def s1(q):
        if q == 0:
            rhs = wout_ref[...]
        elif q == half:
            rhs = wout_all[lax.rem(z + half, n)]
        else:
            rhs = jnp.concatenate([wout_all[lax.rem(z - q + n, n)], wout_all[lax.rem(z + q, n)]], axis=1)
        wq = width(q)
        away = jnp.dot(hidden[oc].reshape(4 * tb, ff), rhs, preferred_element_type=F32)
        s1_send[q, :, :, :wq] = away.astype(BF16).reshape(4, tb, wq)
        kept = jnp.dot(hidden[c].reshape(4 * tb, ff), rhs, preferred_element_type=F32)
        s1_keep[q, :, :, :wq] = kept.reshape(4, tb, wq)

    def s1_copy(q):
        return remote(s1_send.at[q, :, :, w_slice(q)], d_recv.at[q, :, :, w_slice(q)], s1s.at[q], s1r.at[q], sib)

    def chip_sum(q, chip, h):
        part = pl.ds(h * hb, hb)
        wq = width(q)
        return s1_keep[q, chip, part, :wq] + d_recv[q, chip, part, :wq].astype(F32)

    def x_copy(q, kind):
        src, dst, dev = ((r1_send, l1_recv, x_right), (l1_send, r1_recv, x_left),
                         (r2_send, l2_recv, x_right), (l2_send, r2_recv, x_left))[kind]
        if kind < 2:
            src, dst = src.at[q, :, :, w_slice(q)], dst.at[q, :, :, w_slice(q)]
        else:
            src, dst = src.at[q, :, w_slice(q)], dst.at[q, :, w_slice(q)]
        return remote(src, dst, xs.at[kind, q], xr.at[kind, q], dev)

    def s2(q):
        s1_copy(q).wait_recv()
        wq = width(q)
        r1_send[q, 0, :, :wq] = chip_sum(q, xf_, 0).astype(BF16)
        r1_send[q, 1, :, :wq] = chip_sum(q, xr_, 1).astype(BF16)
        l1_send[q, 0, :, :wq] = chip_sum(q, xf_, 1).astype(BF16)
        l1_send[q, 1, :, :wq] = chip_sum(q, xl_, 0).astype(BF16)

    def s3(q):
        wq = width(q)
        x_copy(q, 0).wait_recv()
        r2_send[q, :, :wq] = (chip_sum(q, xr_, 0) + l1_recv[q, 0, :, :wq].astype(F32)).astype(BF16)
        x_copy(q, 1).wait_recv()
        l2_send[q, :, :wq] = (chip_sum(q, xl_, 1) + r1_recv[q, 0, :, :wq].astype(F32)).astype(BF16)

    def s4(q):
        wq = width(q)
        x_copy(q, 2).wait_recv()
        x_copy(q, 3).wait_recv()
        top = chip_sum(q, x, 0) + l2_recv[q, :, :wq].astype(F32) + r1_recv[q, 1, :, :wq].astype(F32)
        low = chip_sum(q, x, 1) + l1_recv[q, 1, :, :wq].astype(F32) + r2_recv[q, :, :wq].astype(F32)
        blocks = (z,) if q == 0 else (lax.rem(z + half, n),) if q == half else (lax.rem(z - q + n, n), lax.rem(z + q, n))
        for i, s in enumerate(blocks):
            cols = pl.ds(pl.multiple_of(s * cb, cb), cb)
            for h, part in ((0, top), (1, low)):
                rws = slice(h * hb, (h + 1) * hb)
                val = tok_ref[rws, cols].astype(F32) + part[:, i * cb:(i + 1) * cb]
                out_ref[rws, cols] = val.astype(BF16)

    def out_slot(s):
        if 0 <= s - 2 <= half:
            s2(s - 2)
        if 0 <= s - 3 <= half:
            s3(s - 3)
        if 0 <= s - 2 <= half:
            go(x_copy(s - 2, 0))
            go(x_copy(s - 2, 1))
        if 0 <= s - 4 <= half:
            s4(s - 4)
        if 0 <= s - 3 <= half:
            go(x_copy(s - 3, 2))
            go(x_copy(s - 3, 3))
        if 0 <= s - 1 <= half:
            if s > 1:
                share_wait(1, s - 1)
            s1(s - 1)
            go(s1_copy(s - 1))

    here, near, far = (x,), (xl_, xr_), (xf_,)
    when = {0: max(1, half * 3 // 8), 1: max(2, half * 4 // 8), 2: max(3, half * 6 // 8)}
    near_at, far_at = half * 6 // 8, half
    for k in range(1, half + 1):
        ring_slot(0, k)
        if k == half:
            ring_own(1)
        for step in (0, 1, 2):
            if when[step] == k:
                tok_slot(step)
        if k > 1:
            share_wait(0, k - 1)
        if k == 2:
            sib_own(oc).wait_recv()
        if k >= 2:
            pre_add(here, 1 if k == 2 else k - 1, k)
        if k == near_at:
            tok_wait(0)
            tok_wait(1)
        if k >= near_at:
            pre_add(near, 1 if k == near_at else k - 1, k)
        if k == far_at:
            tok_wait(2)
            pre_add(far, 1, k)
    for k in range(1, half + 1):
        ring_slot(1, k)
        if k == 1:
            share_wait(0, half)
            finish_hidden()
        out_slot(k)
    for s in range(half + 1, half + 5):
        out_slot(s)
    for copy in started:
        copy.wait_send()


def local(n, tokens, norm_gain, w_in, w_out):
    tb, d = tokens.shape
    kb, ff = w_in.shape
    cb = w_out.shape[1]
    half = n // 2
    q = half + 1
    dma = pltpu.SemaphoreType.DMA
    return pl.pallas_call(
        functools.partial(kernel, n),
        out_shape=jax.ShapeDtypeStruct((tb, d), BF16),
        in_specs=[pl.BlockSpec(memory_space=pltpu.VMEM)] * 4,
        out_specs=pl.BlockSpec(memory_space=pltpu.VMEM),
        scratch_shapes=[
            pltpu.VMEM((2, 4, tb, d), BF16),
            pltpu.VMEM((n, kb, ff), BF16),
            pltpu.VMEM((n, ff, cb), BF16),
            pltpu.VMEM((2, 4, tb, ff), F32),
            pltpu.VMEM((2, 4, tb, ff), BF16),
            pltpu.VMEM((q, 4, tb, 2 * cb), BF16),
            pltpu.VMEM((q, 4, tb, 2 * cb), F32),
            pltpu.VMEM((q, 4, tb, 2 * cb), BF16),
            pltpu.VMEM((q, 2, tb // 2, 2 * cb), BF16),
            pltpu.VMEM((q, 2, tb // 2, 2 * cb), BF16),
            pltpu.VMEM((q, 2, tb // 2, 2 * cb), BF16),
            pltpu.VMEM((q, 2, tb // 2, 2 * cb), BF16),
            pltpu.VMEM((q, tb // 2, 2 * cb), BF16),
            pltpu.VMEM((q, tb // 2, 2 * cb), BF16),
            pltpu.VMEM((q, tb // 2, 2 * cb), BF16),
            pltpu.VMEM((q, tb // 2, 2 * cb), BF16),
            dma((2, 2, half, 2)), dma((2, 2, half, 2)),
            dma((2, 2, half)), dma((2, 2, half)),
            dma((2, 3)), dma((2, 3)),
            dma((2, 4)), dma((2, 4)),
            dma((q,)), dma((q,)),
            dma((4, q)), dma((4, q)),
        ],
        compiler_params=pltpu.CompilerParams(collective_id=0, has_side_effects=True),
    )(tokens, norm_gain.reshape(1, d), w_in, w_out)


def solution(mesh):
    in_specs = (P(("grp", "fs", "tp"), None), P(), P("fs", "tp"), P("tp", "fs"))
    out_specs = P(("grp", "fs", "tp"), None)
    return jax.shard_map(functools.partial(local, mesh.shape["fs"]), mesh=mesh, in_specs=in_specs,
                         out_specs=out_specs, check_vma=False)
```
